32 devices in a mesh: sp: 8 (over z, y), tp: 4 (over x, core).
Axes of the slice: x: 2, y: 2, z: 4, core: 2. Of those that a mesh axis runs over, the one named last changes fastest.
Arguments:
- residual_in: bfloat16 [16384, 2048], P(('sp', 'tp')), may hold values from -6 to 6
- conv_input: bfloat16 [16384, 1024], P('sp', 'tp'), may hold values from -6 to 6
- input_gate: bfloat16 [16384, 1024], P('sp', 'tp'), may hold values from -6 to 6
- output_gate: bfloat16 [16384, 1024], P('sp', 'tp'), may hold values from -6 to 6
- conv_taps: bfloat16 [3, 1024], P(None, 'tp'), may hold values from -3.5 to 3.5
- doc_ids: int32 [16384], P('sp'), may hold values from 0 to 3, never falling along the last dimension, each value on 1 to 8192 neighbouring positions
- proj_weight: bfloat16 [1024, 2048], replicated, may hold values from -0.1875 to 0.1875
- norm_gain: float32 [2048], replicated, may hold values from 0.1 to 1.9
- expert_ids: int32 [16384, 2], P(('sp', 'tp')), may hold values from 0 to 31, all different within a row; in each aligned block of 512 rows (0 to 511, 512 to 1023, ...) at most 64 rows name the same one
- expert_weight: float32 [16384, 2], P(('sp', 'tp')), may hold values from 0.05 to 1
- w_gate: bfloat16 [32, 2048, 512], P('sp'), may hold values from -0.125 to 0.125
- w_up: bfloat16 [32, 2048, 512], P('sp'), may hold values from -0.125 to 0.125
- w_down: bfloat16 [32, 512, 2048], P('sp'), may hold values from -0.25 to 0.25
Outputs:
- layer_out: bfloat16 [16384, 2048], P(('sp', 'tp'))
The draws below stay inside these ranges and needn't reach their ends.
Inputs may be any that keep to these rules, and one draw needn't show every extreme that they name: `doc_ids`: numbers never fall along the sequence; one document spans at most 8192 positions. `expert_ids`: a token's two experts differ; in each aligned block of rows that one device holds, no expert is named more than 64 times, a bound that some block reaches.
All inputs are finite; a program needn't handle non-finite values.
Results may differ from the reference program's by a relative error of at most 0.0047.
Values may be sent and summed in bfloat16 or wider, within the bound.
A program may use at most 128 MiB of HBM per device.

```python
import math
import jax
import jax.numpy as jnp
import numpy as np
from jax import lax

D = 2048
CONV = 1024
FFE = 512
EXPERTS = 32
KW = 3
CAP = 64
TOK_DEV = 2048
TOKENS = 16384
SEG_COUNT = 4
DOC_MOST = 8192
N_SP = 8
N_TP = 4


def block_scale(rng, dims, cuts, smallest, high):
    def one(dim, parts):
        heights = jax.random.uniform(jax.random.fold_in(jax.random.fold_in(rng, 6), dim), (parts,), jnp.float32, smallest / len(cuts), high / len(cuts))
        return jnp.repeat(jnp.exp(heights), dims[dim] // parts).reshape((-1,) + (1,) * (len(dims) - dim - 1))

    loudness = one(*cuts[0])
    for cut in cuts[1:]:
        loudness = loudness * one(*cut)
    return loudness


def profile(amount, total, limit, skew):
    loads = [(1 << 20) // math.isqrt(grade ** skew) + 1 for grade in range(2, amount + 1)]
    surplus, holding = total - limit - (amount - 1), [1] * (amount - 1)
    while surplus > 0:
        free = [i for i in range(amount - 1) if holding[i] < limit]
        mass, budget = sum([loads[i] for i in free]), surplus
        for i in free:
            more = min(limit - holding[i], max(1, budget * loads[i] // mass), surplus)
            holding[i] = holding[i] + more
            surplus = surplus - more
    return np.array([limit] + holding)


def ragged_sizes(stream_key, number_of, total, reach, skew):
    if number_of == 2:
        one = jax.random.randint(stream_key, (), max(1, total - reach), min(reach, total - 1) + 1)
        return jnp.stack([one, total - one])
    sizes = jnp.asarray(profile(number_of, total, reach, skew), jnp.int32)
    couples = (number_of - 1) // 2
    giver, receiver = sizes[1:1 + 2 * couples:2], sizes[2:2 + 2 * couples:2]
    room = jnp.minimum(giver - 1, reach - receiver)
    moved = jax.random.randint(jax.random.fold_in(stream_key, 1), (couples,), 0, 1 << 20) % (room + 1)
    sizes = sizes.at[1:1 + 2 * couples:2].set(giver - moved).at[2:2 + 2 * couples:2].set(receiver + moved)
    return sizes[jax.random.permutation(jax.random.fold_in(stream_key, 2), number_of)]


def assign_block(rng, own, number, rows, number_of, top, bound, lean):
    ranking = jax.random.permutation(rng, number_of)
    packed, common = shares(number_of, rows * top, bound, lean, True), shares(number_of, rows * top, bound, lean, False)
    places = jnp.arange(number_of)

    def named(sizes, turn):
        used = int((sizes > 0).sum())
        fixed = max(1, used // 4)
        passed = fixed + (places - fixed + turn * (used - fixed)) % max(1, number_of - fixed)
        return jnp.zeros((number_of,), jnp.int32).at[ranking[jnp.where(places < fixed, places, passed)]].set(jnp.asarray(sizes, jnp.int32))

    sizes = jnp.where(number % 4 == 0, named(packed, number // 4), named(common, number - number // 4 - 1))
    mixed = jax.random.permutation(jax.random.fold_in(own, 3), number_of)
    donor, taker = mixed[0:number_of // 2 * 2:2], mixed[1:number_of // 2 * 2:2]
    slack = jnp.minimum(sizes[donor] - 1, bound - sizes[taker]) // 2
    slack = jnp.where((donor == ranking[0]) | (taker == ranking[0]) | (sizes[taker] == 0), 0, jnp.maximum(slack, 0))
    passed = jax.random.randint(jax.random.fold_in(own, 4), (number_of // 2,), 0, 1 << 20) % (slack + 1)
    sizes = sizes.at[donor].add(-passed).at[taker].add(passed)
    labels = jnp.searchsorted(jnp.cumsum(sizes), jnp.arange(rows * top), side="right").astype(jnp.int32)
    listing = labels.reshape(top, rows).T
    listing = listing[jax.random.permutation(jax.random.fold_in(own, 1), rows)]
    turn = jax.random.randint(jax.random.fold_in(own, 2), (rows, 1), 0, top)
    return jnp.take_along_axis(listing, (jnp.arange(top)[None, :] + turn) % top, axis=1)


def shares(amount, total, most, skew, full):
    weights = [(1 << 20) // math.isqrt(standing ** skew) + 1 for standing in range(1, amount + 1)]
    largest = most if full else min(most, max(-(-total // amount), total * weights[0] // sum(weights)))
    least = 1 if total - largest >= amount - 1 else 0
    counts, spare = [largest] + [least] * (amount - 1), total - largest - least * (amount - 1)
    while spare > 0:
        movable = [i for i in range(1, amount) if counts[i] < largest] or [i for i in range(1, amount) if counts[i] < most]
        mass, budget = sum([weights[i] for i in movable]), spare
        for i in movable:
            addition = min(most - counts[i], max(1, budget * weights[i] // mass), spare)
            counts[i] = counts[i] + addition
            spare = spare - addition
    return np.array(counts)


def centred(rng, extent, width, most, split=(), kind=jnp.bfloat16):
    values = width * jax.random.normal(rng, extent, jnp.float32)
    if split:
        values = values * block_scale(rng, extent, split, -0.22, 0.18)
    return jnp.clip(values, -most, most).astype(kind)


def setup_inputs(seed: int = 0) -> dict:
    key_of = jax.random.split(jax.random.key(seed), 14)
    residual_in = centred(key_of[0], (TOKENS, D), 1.0, 6.0, ((0, 32),))
    conv_input = centred(key_of[1], (TOKENS, CONV), 1.0, 6.0, ((0, 8), (1, 4)))
    input_gate = centred(key_of[2], (TOKENS, CONV), 1.0, 6.0, ((0, 8), (1, 4)))
    output_gate = centred(key_of[3], (TOKENS, CONV), 1.0, 6.0, ((0, 8), (1, 4)))
    conv_taps = centred(key_of[4], (KW, CONV), KW ** -0.5, 3.5, ((1, 4),))
    doc_ids = jnp.searchsorted(jnp.cumsum(ragged_sizes(key_of[5], SEG_COUNT, TOKENS, DOC_MOST, 2)), jnp.arange(TOKENS), side="right").astype(jnp.int32)
    proj_weight = centred(key_of[6], (CONV, D), CONV ** -0.5, 0.1875)
    norm_gain = jnp.clip(1.0 + 0.18 * jax.random.normal(key_of[7], (D,), jnp.float32), 0.1, 1.9)
    expert_ids_keys = jax.random.split(jax.random.fold_in(key_of[8], 1), TOKENS // (TOK_DEV // N_TP))
    expert_ids_turns = jax.random.permutation(jax.random.fold_in(key_of[8], 3), TOKENS // (TOK_DEV // N_TP))
    expert_ids = jax.vmap(lambda own, number: assign_block(jax.random.fold_in(key_of[8], 2), own, number, TOK_DEV // N_TP, EXPERTS, 2, CAP, 2))(expert_ids_keys, expert_ids_turns).reshape((TOKENS, 2))
    expert_weight = jnp.clip(jnp.exp(math.log(1.0) - 2.9957323 * jax.random.uniform(key_of[9], (TOKENS, 2), jnp.float32) ** block_scale(key_of[9], (TOKENS, 2), ((0, 32),), -0.2, 0.2)), 0.05, 1.0)
    w_gate = centred(key_of[10], (EXPERTS, D, FFE), D ** -0.5, 0.125, ((0, 8),))
    w_up = centred(key_of[11], (EXPERTS, D, FFE), D ** -0.5, 0.125, ((0, 8),))
    w_down = centred(key_of[12], (EXPERTS, FFE, D), FFE ** -0.5, 0.25, ((0, 8),))
    return dict(residual_in=residual_in, conv_input=conv_input, input_gate=input_gate, output_gate=output_gate, conv_taps=conv_taps, doc_ids=doc_ids, proj_weight=proj_weight, norm_gain=norm_gain, expert_ids=expert_ids, expert_weight=expert_weight, w_gate=w_gate, w_up=w_up, w_down=w_down)


epsilon = 1e-06

def reference(residual_in, conv_input, input_gate, output_gate, conv_taps, doc_ids, proj_weight, norm_gain, expert_ids, expert_weight, w_gate, w_up, w_down):
    product = input_gate.astype(jnp.float32) * conv_input.astype(jnp.float32)
    padded_in = jnp.concatenate([jnp.zeros((KW - 1, CONV), jnp.float32), product], axis=0)
    padded_ids = jnp.concatenate([jnp.full((KW - 1,), -1, jnp.int32), doc_ids.astype(jnp.int32)], axis=0)
    conv_sum = jnp.zeros((TOKENS, CONV), jnp.float32)
    for offset in range(KW):
        same_doc = padded_ids[offset:offset + TOKENS] == doc_ids
        term = conv_taps[offset].astype(jnp.float32)[None, :] * padded_in[offset:offset + TOKENS]
        conv_sum = conv_sum + jnp.where(same_doc[:, None], term, 0.0)
    gated = (output_gate.astype(jnp.float32) * conv_sum).astype(jnp.bfloat16)
    hidden = residual_in.astype(jnp.float32) + jnp.dot(gated, proj_weight, preferred_element_type=jnp.float32)
    scale_rows = lax.rsqrt(lax.optimization_barrier(jnp.mean(hidden * hidden, axis=-1, keepdims=True)) + epsilon)
    normed = (hidden * scale_rows * norm_gain[None, :]).astype(jnp.bfloat16)
    blocks = N_SP * N_TP
    block_rows = TOK_DEV // N_TP
    slots_all = blocks * CAP
    flat_ids = expert_ids.reshape(blocks, 2 * block_rows)
    one_hot = (flat_ids[:, :, None] == jnp.arange(EXPERTS, dtype=jnp.int32)[None, None, :]).astype(jnp.int32)
    before = jnp.cumsum(one_hot, axis=1) - one_hot
    slot_num = lax.optimization_barrier(jnp.sum(before * one_hot, axis=-1))
    slot_index = (jnp.arange(blocks, dtype=jnp.int32)[:, None] * CAP + slot_num).reshape(TOKENS, 2).astype(jnp.int32)

    def per_expert(total, expert):
        chosen = expert_ids == expert
        target = jnp.where(chosen, slot_index, slots_all)
        buffer = jnp.zeros((slots_all, D), jnp.bfloat16)
        buffer = buffer.at[target[:, 0]].set(normed, mode='drop')
        buffer = buffer.at[target[:, 1]].set(normed, mode='drop')
        gate_val = jnp.dot(buffer, w_gate[expert], preferred_element_type=jnp.float32)
        up_val = jnp.dot(buffer, w_up[expert], preferred_element_type=jnp.float32)
        act_rows = (jax.nn.silu(gate_val) * up_val).astype(jnp.bfloat16)
        out_rows = jnp.dot(act_rows, w_down[expert], preferred_element_type=jnp.float32).astype(jnp.bfloat16)
        for route in range(2):
            picked = out_rows[slot_index[:, route]].astype(jnp.float32) * expert_weight[:, route:route + 1]
            total = total + jnp.where(chosen[:, route:route + 1], picked, 0.0)
        return (total, None)
    expert_sum, unused = lax.scan(per_expert, jnp.zeros((TOKENS, D), jnp.float32), jnp.arange(EXPERTS, dtype=jnp.int32))
    return (hidden + expert_sum).astype(jnp.bfloat16)
```

```python
import functools

import jax
import jax.numpy as jnp
from jax import lax
from jax.experimental import pallas as pl
from jax.experimental.pallas import tpu as pltpu
from jax.sharding import PartitionSpec as P

CAP = 64
PLANES = 4
CHUNKS = 4
BLOCK = 128
HALF = 256
epsilon = 1e-06
MESH = pl.DeviceIdType.MESH
bf16, f32 = jnp.bfloat16, jnp.float32


def lookup(table, p, k):
    out = 0
    for i, row in enumerate(table):
        for j, v in enumerate(row):
            out = out + jnp.where((p == i) & (k == j), v, 0)
    return out


ORDER = ((0, 1, 2, 3), (1, 0, 2, 3), (2, 3, 1, 0), (3, 2, 1, 0))
LOW = ((0, 1, 2, 3), (0, 1, 3, 3), (0, 1, 3, 3), (0, 1, 2, 3))
HIGH = ((1, 2, 3, 4), (1, 3, 3, 4), (1, 3, 3, 4), (1, 2, 3, 4))


def moe_kernel(
    rest,
    normed_hbm,
    meta_hbm,
    hidden_hbm,
    gate_hbm,
    up_hbm,
    down_hbm,
    out_hbm,
    tok,
    meta,
    slots,
    away,
    back,
    parts,
    gate,
    up,
    down,
    pick,
    mix,
    hid,
    fin,
    load_sem,
    meta_load_sem,
    weight_sem,
    own_sem,
    own_meta_sem,
    tok_send,
    tok_recv,
    meta_send,
    meta_recv,
    away_send,
    away_recv,
    back_send,
    back_recv,
    part_send,
    part_recv,
    hid_sem,
    fin_sem,
):
    me = lax.axis_index("sp")
    p, r = me // rest, lax.rem(me, rest)
    first, last = p == 0, p == PLANES - 1
    inner = jnp.logical_not(first | last)
    below = lax.max(me - rest, 0)
    above = lax.min(me + rest, PLANES * rest - 1)
    experts, _, hidden_width = gate.shape
    tokens, width = tok.shape[2], tok.shape[3]
    local = experts * CAP
    peers = [p * rest + lax.rem(r + d, rest) for d in range(1, rest)]
    origins = [p * rest + lax.rem(r + rest - d, rest) for d in range(1, rest)]

    def remote(src, dst, send, recv, device):
        return pltpu.make_async_remote_copy(
            src_ref=src, dst_ref=dst, send_sem=send, recv_sem=recv, device_id={"sp": device}, device_id_type=MESH
        )

    def token_copy(s, c, send, device):
        return remote(tok.at[s, c], tok.at[s, c], send, tok_recv.at[s, c], device)

    def meta_copy(s, send, device):
        return remote(meta.at[s], meta.at[s], send, meta_recv.at[s], device)

    def away_copy(s, d, c):
        peer = peers[d]
        return remote(slots.at[s, lax.rem(r + d + 1, rest), c], away.at[s, d, c], away_send.at[s, d, c], away_recv.at[s, d, c], peer)

    def back_copy(s, d, e):
        return remote(away.at[s, d, :, e], back.at[s, d, :, e], back_send.at[s, d, e], back_recv.at[s, d, e], origins[d])

    def part_copy(s, c):
        down_way = p > s
        target = jnp.where(down_way, below, above)
        index = jnp.where(down_way & (p - 1 == s), PLANES, s)
        return remote(tok.at[s, c], parts.at[index, c], part_send.at[s, c], part_recv.at[index, c], target)

    def part_arrival(index, c):
        return remote(tok.at[0, c], parts.at[index, c], part_send.at[0, c], part_recv.at[index, c], below)

    loads = [
        pltpu.make_async_copy(normed_hbm.at[:, pl.ds(c * width, width)], tok.at[p, c], load_sem.at[c]) for c in range(CHUNKS)
    ]
    meta_load = pltpu.make_async_copy(meta_hbm, meta.at[p], meta_load_sem)

    def weight_copies(e):
        pairs = ((gate_hbm, gate), (up_hbm, up), (down_hbm, down))
        return [pltpu.make_async_copy(a.at[e], b.at[e], weight_sem.at[i, e]) for i, (a, b) in enumerate(pairs)]

    meta_load.start()
    for load in loads:
        load.start()
    barrier = pltpu.get_barrier_semaphore()

    @pl.when(jnp.logical_not(first))
    def _():
        pl.semaphore_signal(barrier, inc=1, device_id={"sp": below}, device_id_type=MESH)

    @pl.when(jnp.logical_not(last))
    def _():
        pl.semaphore_signal(barrier, inc=1, device_id={"sp": above}, device_id_type=MESH)

    for peer in peers:
        pl.semaphore_signal(barrier, inc=1, device_id={"sp": peer}, device_id_type=MESH)
    pl.semaphore_wait(barrier, rest - 1 + jnp.where(inner, 2, 1))

    def own_copy(way, c):
        device = (above, below)[way]
        if c == 0:
            return meta_copy(p, own_meta_sem.at[way], device)
        return token_copy(p, c - 1, own_sem.at[way, c - 1], device)

    ways = (jnp.logical_not(last), jnp.logical_not(first))
    meta_load.wait()
    for c in range(CHUNKS + 1):
        if c:
            loads[c - 1].wait()
        for way in range(2):

            @pl.when(ways[way])
            def _():
                own_copy(way, c).start()

    for e in range(experts):
        for copy in weight_copies(e):
            copy.start()

    def unpack_step(k, carry):
        s = lookup(ORDER, p, k)
        onward = jnp.where(s < p, above, below)
        fresh = k > 0

        @pl.when(fresh)
        def _():
            meta_copy(s, meta_send.at[s], onward).wait_recv()

        @pl.when(fresh & inner)
        def _():
            meta_copy(s, meta_send.at[s], onward).start()

        def pick_rows(q, carry):
            base = (p * rest * local + q * BLOCK).astype(f32)
            names = lax.broadcasted_iota(jnp.int32, (BLOCK, tokens), 0).astype(f32)
            hit = (names == meta[s, 0:1] - base) | (names == meta[s, 1:2] - base)
            pick[pl.ds(pl.multiple_of(q * BLOCK, BLOCK), BLOCK), :] = jnp.where(hit, 1.0, 0.0).astype(bf16)
            return carry

        lax.fori_loop(0, rest * local // BLOCK, pick_rows, 0)

        def chunk(c, carry):
            @pl.when(fresh)
            def _():
                token_copy(s, c, tok_send.at[s, c], onward).wait_recv()

            @pl.when(fresh & inner)
            def _():
                token_copy(s, c, tok_send.at[s, c], onward).start()

            def pack(q, carry):
                chosen = pick[pl.ds(pl.multiple_of(q * local, local), local), :]
                rows = jnp.dot(chosen, tok[s, c], preferred_element_type=f32).astype(bf16)
                slots[s, q, c] = rows.reshape(experts, CAP, width)
                return carry

            lax.fori_loop(0, rest, pack, 0)
            for d in range(rest - 1):
                away_copy(s, d, c).start()
            return carry

        return lax.fori_loop(0, CHUNKS, chunk, carry)

    def expert_step(k):
        s = lookup(ORDER, p, k)
        for d in range(rest - 1):
            for c in range(CHUNKS):
                away_copy(s, d, c).wait_recv()

        def one(e, carry):
            @pl.when(k == 0)
            def _():
                for copy in weight_copies(e):
                    copy.wait()

            gate_val = jnp.zeros((rest * CAP, hidden_width), f32)
            up_val = jnp.zeros((rest * CAP, hidden_width), f32)
            for c in range(CHUNKS):
                x = jnp.concatenate([slots[s, r, c, e]] + [away[s, d, c, e] for d in range(rest - 1)], axis=0)
                rows = pl.ds(c * width, width)
                gate_val = gate_val + jnp.dot(x, gate[e, rows, :], preferred_element_type=f32)
                up_val = up_val + jnp.dot(x, up[e, rows, :], preferred_element_type=f32)
            act = (gate_val * jax.nn.sigmoid(gate_val) * up_val).astype(bf16)
            for c in range(CHUNKS):
                out = jnp.dot(act, down[e, :, pl.ds(c * width, width)], preferred_element_type=f32).astype(bf16)
                slots[s, r, c, e] = out[:CAP]
                for d in range(rest - 1):
                    away[s, d, c, e] = out[(d + 1) * CAP : (d + 2) * CAP]
            for d in range(rest - 1):
                back_copy(s, d, e).start()
            return carry

        lax.fori_loop(0, experts, one, 0)

    def make_mix(s, i):
        def rows(q, carry):
            here = pl.ds(pl.multiple_of(q * BLOCK, BLOCK), BLOCK)
            info = meta[s, :, here].T
            names = lax.broadcasted_iota(jnp.int32, (BLOCK, local), 1).astype(f32)
            for d in range(rest):
                base = (p * rest * local + lax.rem(r + d, rest) * local).astype(f32)
                mix[i, d, here] = (
                    jnp.where(names == info[:, 0:1] - base, info[:, 2:3], 0.0)
                    + jnp.where(names == info[:, 1:2] - base, info[:, 3:4], 0.0)
                ).astype(bf16)
            return carry

        lax.fori_loop(0, tokens // BLOCK, rows, 0)

    def returns(s):
        for d in range(rest - 1):
            for e in range(experts):
                back_copy(s, d, e).wait_recv()

    def combine(s, i, c, here):
        acc = jnp.dot(mix[i, 0, here], slots[s, r, c].reshape(local, width), preferred_element_type=f32)
        for d in range(rest - 1):
            acc = acc + jnp.dot(mix[i, d + 1, here], back[s, d, c].reshape(local, width), preferred_element_type=f32)
        return acc

    def by_rows(step):
        def body(q, carry):
            step(pl.ds(pl.multiple_of(q * HALF, HALF), HALF))
            return carry

        lax.fori_loop(0, tokens // HALF, body, 0)

    def send_part(s, i, c, passed):
        if passed:
            part_arrival(s, c).wait_recv()
            token_copy(s, c, tok_send.at[s, c], below).wait_send()

        def step(here):
            acc = combine(s, i, c, here)
            if passed:
                acc = acc + parts[s, c, here].astype(f32)
            tok[s, c, here] = acc.astype(bf16)

        by_rows(step)
        part_copy(s, c).start()

    def main_step(k, carry):
        lax.fori_loop(lookup(LOW, p, k), lookup(HIGH, p, k), unpack_step, 0)
        expert_step(k)

        @pl.when((k > 0) & jnp.logical_not(inner))
        def _():
            s = lookup(ORDER, p, k)
            returns(s)
            make_mix(s, 0)

            def chunk(c, carry):
                send_part(s, 0, c, False)
                return carry

            lax.fori_loop(0, CHUNKS, chunk, 0)

        return carry

    lax.fori_loop(0, PLANES, main_step, 0)

    @pl.when(inner)
    def _():
        near = PLANES - 1 - p
        end = jnp.where(p == 1, PLANES - 1, 0)
        far = PLANES - 1 - end
        returns(near)
        make_mix(near, 0)

        def one(c, carry):
            send_part(near, 0, c, True)
            return carry

        lax.fori_loop(0, CHUNKS, one, 0)
        returns(end)
        returns(far)
        make_mix(end, 0)
        make_mix(far, 1)

        def two(c, carry):
            send_part(end, 0, c, True)
            send_part(far, 1, c, True)
            return carry

        lax.fori_loop(0, CHUNKS, two, 0)

    def fin_copy(c):
        return pltpu.make_async_copy(fin.at[c % 2], out_hbm.at[:, pl.ds(c * width, width)], fin_sem.at[c % 2])

    returns(p)
    make_mix(p, 0)
    for c in range(CHUNKS):
        hid_copy = pltpu.make_async_copy(hidden_hbm.at[:, pl.ds(c * width, width)], hid, hid_sem)
        hid_copy.start()
        hid_copy.wait()

        @pl.when(jnp.logical_not(first))
        def _():
            part_arrival(p, c).wait_recv()

            def step(here):
                hid[here] = hid[here] + parts[p, c, here].astype(f32)

            by_rows(step)

        @pl.when(jnp.logical_not(last))
        def _():
            part_arrival(PLANES, c).wait_recv()

            def step(here):
                hid[here] = hid[here] + parts[PLANES, c, here].astype(f32)

            by_rows(step)

        def step(here):
            fin[c % 2, here] = (hid[here] + combine(p, 0, c, here)).astype(bf16)

        by_rows(step)
        fin_copy(c).start()
        if c:
            fin_copy(c - 1).wait()
    fin_copy(CHUNKS - 1).wait()

    for way in range(2):

        @pl.when(ways[way])
        def _():
            for c in range(CHUNKS + 1):
                own_copy(way, c).wait_send()

    def drain(k, carry):
        s = lookup(ORDER, p, k)
        for d in range(rest - 1):
            for c in range(CHUNKS):
                away_copy(s, d, c).wait_send()
            for e in range(experts):
                back_copy(s, d, e).wait_send()

        @pl.when(k > 0)
        def _():
            for c in range(CHUNKS):
                part_copy(s, c).wait_send()

        @pl.when((k > 0) & inner)
        def _():
            meta_copy(s, meta_send.at[s], below).wait_send()

        return carry

    lax.fori_loop(0, PLANES, drain, 0)


def experts_and_back(normed, meta, hidden, w_gate, w_up, w_down):
    rest = lax.axis_size("sp") // PLANES
    experts, model, ffe = w_gate.shape
    tokens = normed.shape[0]
    width = model // CHUNKS
    dma = pltpu.SemaphoreType.DMA
    anywhere = pl.BlockSpec(memory_space=pl.ANY)
    return pl.pallas_call(
        functools.partial(moe_kernel, rest),
        in_specs=[anywhere] * 6,
        out_specs=anywhere,
        out_shape=jax.ShapeDtypeStruct((tokens, model), bf16),
        scratch_shapes=[
            pltpu.VMEM((PLANES, CHUNKS, tokens, width), bf16),
            pltpu.VMEM((PLANES,) + meta.shape, f32),
            pltpu.VMEM((PLANES, rest, CHUNKS, experts, CAP, width), bf16),
            pltpu.VMEM((PLANES, rest - 1, CHUNKS, experts, CAP, width), bf16),
            pltpu.VMEM((PLANES, rest - 1, CHUNKS, experts, CAP, width), bf16),
            pltpu.VMEM((PLANES + 1, CHUNKS, tokens, width), bf16),
            pltpu.VMEM(w_gate.shape, bf16),
            pltpu.VMEM(w_up.shape, bf16),
            pltpu.VMEM(w_down.shape, bf16),
            pltpu.VMEM((rest * experts * CAP, tokens), bf16),
            pltpu.VMEM((2, rest, tokens, experts * CAP), bf16),
            pltpu.VMEM((tokens, width), f32),
            pltpu.VMEM((2, tokens, width), bf16),
            dma((CHUNKS,)),
            dma,
            dma((3, experts)),
            dma((2, CHUNKS)),
            dma((2,)),
            dma((PLANES, CHUNKS)),
            dma((PLANES, CHUNKS)),
            dma((PLANES,)),
            dma((PLANES,)),
            dma((PLANES, rest - 1, CHUNKS)),
            dma((PLANES, rest - 1, CHUNKS)),
            dma((PLANES, rest - 1, experts)),
            dma((PLANES, rest - 1, experts)),
            dma((PLANES, CHUNKS)),
            dma((PLANES + 1, CHUNKS)),
            dma,
            dma((2,)),
        ],
        compiler_params=pltpu.CompilerParams(collective_id=0, has_side_effects=True, vmem_limit_bytes=67043328),
        cost_estimate=pl.CostEstimate(
            flops=6 * PLANES * rest * experts * CAP * model * ffe,
            bytes_accessed=2 * (w_gate.size * 3 + 4 * normed.size),
            transcendentals=PLANES * rest * experts * CAP * ffe,
        ),
    )(normed, meta, hidden, w_gate, w_up, w_down)


def from_behind(x, axis, by):
    devices = lax.axis_size(axis)
    pairs = [(i, i + by) for i in range(devices) if 0 <= i + by < devices]
    return lax.ppermute(x, axis, pairs)


def slot_table(ids, weights, experts):
    tokens = ids.shape[1]
    names = jnp.arange(experts, dtype=jnp.int32)[:, None]
    hits = [ids[j][None, :] == names for j in range(2)]
    named = (hits[0] | hits[1]).astype(bf16)
    at = jnp.arange(tokens, dtype=jnp.int32)
    earlier = (at[:, None] < at[None, :]).astype(bf16)
    before = jnp.dot(named, earlier, preferred_element_type=f32)
    rank = [jnp.sum(jnp.where(hits[j], before, 0.0), axis=0) for j in range(2)]
    slot = [ids[j].astype(f32) * CAP + rank[j] for j in range(2)]
    return jnp.concatenate([jnp.stack(slot), weights, jnp.zeros((4, tokens), f32)], axis=0)


def per_device(
    residual_in,
    conv_input,
    input_gate,
    output_gate,
    conv_taps,
    doc_ids,
    proj_weight,
    norm_gain,
    expert_ids,
    expert_weight,
    w_gate,
    w_up,
    w_down,
):
    kernel_width = conv_taps.shape[0]
    rim_rows = kernel_width - 1
    meta = slot_table(expert_ids.T, expert_weight.T, w_gate.shape[0] * lax.axis_size("sp"))

    product = input_gate.astype(f32) * conv_input.astype(f32)
    doc_float = doc_ids.astype(f32)
    doc_rim = jnp.broadcast_to(doc_float[-rim_rows:, None], (rim_rows, 128))
    rim = from_behind(jnp.concatenate([product[-rim_rows:], doc_rim], axis=1), "sp", 1)
    channels = product.shape[1]
    prev_in, prev_ids = rim[:, :channels], rim[:, channels]
    prev_ids = jnp.where(lax.axis_index("sp") == 0, -1.0, prev_ids)
    padded_in = jnp.concatenate([prev_in, product], axis=0)
    padded_ids = jnp.concatenate([prev_ids, doc_float], axis=0)
    length = product.shape[0]
    conv_sum = jnp.zeros(product.shape, f32)
    for offset in range(kernel_width):
        same_doc = padded_ids[offset : offset + length] == doc_float
        term = conv_taps[offset].astype(f32)[None, :] * padded_in[offset : offset + length]
        conv_sum = conv_sum + jnp.where(same_doc[:, None], term, 0.0)
    gated = (output_gate.astype(f32) * conv_sum).astype(bf16)
    regrouped = lax.all_to_all(gated, "tp", split_axis=0, concat_axis=1, tiled=True)

    mixed = jnp.dot(regrouped, proj_weight, preferred_element_type=f32)
    hidden = residual_in.astype(f32) + mixed
    scale_rows = lax.rsqrt(jnp.mean(hidden * hidden, axis=-1, keepdims=True) + epsilon)
    normed = (hidden * scale_rows * norm_gain[None, :]).astype(bf16)
    return experts_and_back(normed, meta, hidden, w_gate, w_up, w_down)


def solution(mesh):
    return jax.shard_map(
        per_device,
        mesh=mesh,
        in_specs=(
            P(("sp", "tp"), None),
            P("sp", "tp"),
            P("sp", "tp"),
            P("sp", "tp"),
            P(None, "tp"),
            P("sp"),
            P(),
            P(),
            P(("sp", "tp"), None),
            P(("sp", "tp"), None),
            P("sp", None, None),
            P("sp", None, None),
            P("sp", None, None),
        ),
        out_specs=P(("sp", "tp"), None),
        check_vma=False,
    )
```

```python
import functools

import jax
import jax.numpy as jnp
from jax import lax
from jax.experimental import pallas as pl
from jax.experimental.pallas import tpu as pltpu
from jax.sharding import PartitionSpec as P

CAP = 64
PLANES = 4
CHUNKS = 4
BLOCK = 128
HALF = 256
epsilon = 1e-06
MESH = pl.DeviceIdType.MESH
bf16, f32 = jnp.bfloat16, jnp.float32


def lookup(table, p, k):
    out = 0
    for i, row in enumerate(table):
        for j, v in enumerate(row):
            out = out + jnp.where((p == i) & (k == j), v, 0)
    return out


ORDER = ((0, 1, 3, 2), (1, 0, 3, 2), (2, 3, 0, 1), (3, 2, 0, 1))
LOW = ((0, 1, 2, 3), (0, 1, 3, 3), (0, 1, 3, 3), (0, 1, 2, 3))
HIGH = ((1, 2, 2, 3), (1, 3, 3, 4), (1, 3, 3, 4), (1, 2, 2, 3))


def moe_kernel(
    rest,
    normed_hbm,
    meta_hbm,
    hidden_hbm,
    gate_hbm,
    up_hbm,
    down_hbm,
    out_hbm,
    tok,
    meta,
    slots,
    away,
    back,
    parts,
    gate,
    up,
    down,
    pick,
    mix,
    act,
    hid,
    fin,
    load_sem,
    meta_load_sem,
    weight_sem,
    own_sem,
    own_meta_sem,
    tok_send,
    tok_recv,
    meta_send,
    meta_recv,
    away_send,
    away_recv,
    back_send,
    back_recv,
    part_send,
    part_recv,
    hid_sem,
    fin_sem,
):
    me = lax.axis_index("sp")
    p, r = me // rest, lax.rem(me, rest)
    first, last = p == 0, p == PLANES - 1
    inner = jnp.logical_not(first | last)
    below = lax.max(me - rest, 0)
    above = lax.min(me + rest, PLANES * rest - 1)
    experts, _, hidden_width = gate.shape
    tokens, width = tok.shape[2], tok.shape[3]
    local = experts * CAP
    peers = [p * rest + lax.rem(r + d, rest) for d in range(1, rest)]
    origins = [p * rest + lax.rem(r + rest - d, rest) for d in range(1, rest)]

    def remote(src, dst, send, recv, device):
        return pltpu.make_async_remote_copy(
            src_ref=src, dst_ref=dst, send_sem=send, recv_sem=recv, device_id={"sp": device}, device_id_type=MESH
        )

    def token_copy(s, c, send, device):
        return remote(tok.at[s, c], tok.at[s, c], send, tok_recv.at[s, c], device)

    def meta_copy(s, send, device):
        return remote(meta.at[s], meta.at[s], send, meta_recv.at[s], device)

    def away_copy(s, d, c):
        peer = peers[d]
        return remote(slots.at[s, lax.rem(r + d + 1, rest), c], away.at[s, d, c], away_send.at[s, d, c], away_recv.at[s, d, c], peer)

    def back_copy(s, d, c):
        return remote(away.at[s, d, c], back.at[s, d, c], back_send.at[s, d, c], back_recv.at[s, d, c], origins[d])

    def part_copy(s, c):
        down_way = p > s
        target = jnp.where(down_way, below, above)
        index = jnp.where(down_way & (p - 1 == s), PLANES, s)
        return remote(tok.at[s, c], parts.at[index, c], part_send.at[s, c], part_recv.at[index, c], target)

    def part_arrival(index, c):
        return remote(tok.at[0, c], parts.at[index, c], part_send.at[0, c], part_recv.at[index, c], below)

    loads = [
        pltpu.make_async_copy(normed_hbm.at[:, pl.ds(c * width, width)], tok.at[p, c], load_sem.at[c]) for c in range(CHUNKS)
    ]
    meta_load = pltpu.make_async_copy(meta_hbm, meta.at[p], meta_load_sem)

    def weight_copies(e):
        pairs = ((gate_hbm, gate), (up_hbm, up), (down_hbm, down))
        return [pltpu.make_async_copy(a.at[e], b.at[e], weight_sem.at[i, e]) for i, (a, b) in enumerate(pairs)]

    meta_load.start()
    for load in loads:
        load.start()
    barrier = pltpu.get_barrier_semaphore()

    @pl.when(jnp.logical_not(first))
    def _():
        pl.semaphore_signal(barrier, inc=1, device_id={"sp": below}, device_id_type=MESH)

    @pl.when(jnp.logical_not(last))
    def _():
        pl.semaphore_signal(barrier, inc=1, device_id={"sp": above}, device_id_type=MESH)

    for peer in peers:
        pl.semaphore_signal(barrier, inc=1, device_id={"sp": peer}, device_id_type=MESH)
    pl.semaphore_wait(barrier, rest - 1 + jnp.where(inner, 2, 1))

    def own_copy(way, c):
        device = (above, below)[way]
        if c == 0:
            return meta_copy(p, own_meta_sem.at[way], device)
        return token_copy(p, c - 1, own_sem.at[way, c - 1], device)

    ways = (jnp.logical_not(last), jnp.logical_not(first))
    middle = (p == 1, p == PLANES - 2)
    meta_load.wait()
    for c in range(CHUNKS + 1):
        if c:
            loads[c - 1].wait()
        for way in range(2):

            @pl.when(ways[way] if c < 2 else ways[way] & jnp.logical_not(middle[way]))
            def _():
                own_copy(way, c).start()

    for e in range(experts):
        for copy in weight_copies(e):
            copy.start()

    def unpack_start(k):
        s = lookup(ORDER, p, k)
        onward = jnp.where(s < p, above, below)
        fresh = k > 0

        @pl.when(fresh)
        def _():
            meta_copy(s, meta_send.at[s], onward).wait_recv()

        @pl.when(fresh & inner)
        def _():
            meta_copy(s, meta_send.at[s], onward).start()

        def pick_rows(q, carry):
            base = (p * rest * local + q * BLOCK).astype(f32)
            names = lax.broadcasted_iota(jnp.int32, (BLOCK, tokens), 0).astype(f32)
            hit = (names == meta[s, 0:1] - base) | (names == meta[s, 1:2] - base)
            pick[pl.ds(pl.multiple_of(q * BLOCK, BLOCK), BLOCK), :] = jnp.where(hit, 1.0, 0.0).astype(bf16)
            return carry

        lax.fori_loop(0, rest * local // BLOCK, pick_rows, 0)

    def unpack_chunk(k, c):
        s = lookup(ORDER, p, k)
        onward = jnp.where(s < p, above, below)
        fresh = k > 0

        @pl.when(fresh)
        def _():
            token_copy(s, c, tok_send.at[s, c], onward).wait_recv()

        @pl.when(fresh & inner)
        def _():
            token_copy(s, c, tok_send.at[s, c], onward).start()

        def pack(q, carry):
            chosen = pick[pl.ds(pl.multiple_of(q * local, local), local), :]
            rows = jnp.dot(chosen, tok[s, c], preferred_element_type=f32).astype(bf16)
            slots[s, q, c] = rows.reshape(experts, CAP, width)
            return carry

        lax.fori_loop(0, rest, pack, 0)
        for d in range(rest - 1):
            away_copy(s, d, c).start()

    def unpack_step(k, carry):
        unpack_start(k)

        def chunk(c, carry):
            unpack_chunk(k, c)
            return carry

        lax.fori_loop(0, CHUNKS, chunk, 0)
        for way in range(2):

            @pl.when(middle[way] & (k == 1))
            def _():
                for c in range(2, CHUNKS + 1):
                    own_copy(way, c).start()

        return carry

    def expert_step(k):
        s = lookup(ORDER, p, k)
        for d in range(rest - 1):
            for c in range(CHUNKS):
                away_copy(s, d, c).wait_recv()

        def one(e, carry):
            @pl.when(k == 1)
            def _():
                for copy in weight_copies(e):
                    copy.wait()

            gate_val = jnp.zeros((rest * CAP, hidden_width), f32)
            up_val = jnp.zeros((rest * CAP, hidden_width), f32)
            for c in range(CHUNKS):
                x = jnp.concatenate([slots[s, r, c, e]] + [away[s, d, c, e] for d in range(rest - 1)], axis=0)
                rows = pl.ds(c * width, width)
                gate_val = gate_val + jnp.dot(x, gate[e, rows, :], preferred_element_type=f32)
                up_val = up_val + jnp.dot(x, up[e, rows, :], preferred_element_type=f32)
            act[e] = (gate_val * jax.nn.sigmoid(gate_val) * up_val).astype(bf16)
            return carry

        lax.fori_loop(0, experts, one, 0)

        def two(c, carry):
            for e in range(experts):
                columns = pl.ds(pl.multiple_of(c * width, width), width)
                out = jnp.dot(act[e], down[e, :, columns], preferred_element_type=f32).astype(bf16)
                slots[s, r, c, e] = out[:CAP]
                for d in range(rest - 1):
                    away[s, d, c, e] = out[(d + 1) * CAP : (d + 2) * CAP]

            @pl.when(k > 0)
            def _():
                for d in range(rest - 1):
                    back_copy(s, d, c).start()

            return carry

        lax.fori_loop(0, CHUNKS, two, 0)

    def make_mix(s, i):
        def rows(q, carry):
            here = pl.ds(pl.multiple_of(q * BLOCK, BLOCK), BLOCK)
            info = meta[s, :, here].T
            names = lax.broadcasted_iota(jnp.int32, (BLOCK, local), 1).astype(f32)
            for d in range(rest):
                base = (p * rest * local + lax.rem(r + d, rest) * local).astype(f32)
                mix[i, d, here] = (
                    jnp.where(names == info[:, 0:1] - base, info[:, 2:3], 0.0)
                    + jnp.where(names == info[:, 1:2] - base, info[:, 3:4], 0.0)
                ).astype(bf16)
            return carry

        lax.fori_loop(0, tokens // BLOCK, rows, 0)

    def returned(s, c):
        for d in range(rest - 1):
            back_copy(s, d, c).wait_recv()

    def combine(s, i, c, here):
        acc = jnp.dot(mix[i, 0, here], slots[s, r, c].reshape(local, width), preferred_element_type=f32)
        for d in range(rest - 1):
            acc = acc + jnp.dot(mix[i, d + 1, here], back[s, d, c].reshape(local, width), preferred_element_type=f32)
        return acc

    def by_rows(step):
        def body(q, carry):
            step(pl.ds(pl.multiple_of(q * HALF, HALF), HALF))
            return carry

        lax.fori_loop(0, tokens // HALF, body, 0)

    def send_part(s, i, c, passed):
        returned(s, c)
        if passed:
            part_arrival(s, c).wait_recv()
            token_copy(s, c, tok_send.at[s, c], below).wait_send()

        def step(here):
            acc = combine(s, i, c, here)
            if passed:
                acc = acc + parts[s, c, here].astype(f32)
            tok[s, c, here] = acc.astype(bf16)

        by_rows(step)
        part_copy(s, c).start()

    near = jnp.clip(PLANES - 1 - p, 0, PLANES - 1)
    end = jnp.where(p == 1, PLANES - 1, 0)
    far = PLANES - 1 - end

    def main_step(k, carry):
        lax.fori_loop(lookup(LOW, p, k), lookup(HIGH, p, k), unpack_step, 0)

        @pl.when(inner & (k == PLANES - 1))
        def _():
            make_mix(end, 0)
            make_mix(far, 1)
            send_part(end, 0, 0, True)
            send_part(end, 0, 1, True)
            send_part(far, 1, 0, True)

        def expert_turn(i, carry):
            expert_step(jnp.where(i == 0, k, 0))
            return carry

        own_turn = jnp.where(inner, PLANES - 1, 1)
        lax.fori_loop(0, jnp.where(k == own_turn, 2, 1), expert_turn, 0)

        @pl.when(k == PLANES - 1)
        def _():
            for c in range(CHUNKS):
                for d in range(rest - 1):
                    back_copy(p, d, c).start()

        @pl.when(jnp.logical_not(inner))
        def _():
            s = lookup(ORDER, p, k)
            make_mix(s, 0)

            @pl.when(k < PLANES - 1)
            def _():
                unpack_start(k + 1)

            def chunk(c, carry):
                @pl.when(k < PLANES - 1)
                def _():
                    unpack_chunk(k + 1, c)

                send_part(s, 0, c, False)
                return carry

            lax.fori_loop(0, CHUNKS, chunk, 0)

        return carry

    unpack_step(0, 0)
    lax.fori_loop(1, PLANES, main_step, 0)

    @pl.when(inner)
    def _():
        def two(c, carry):
            send_part(end, 0, c, True)
            send_part(far, 1, c - 1, True)
            return carry

        lax.fori_loop(2, CHUNKS, two, 0)
        send_part(far, 1, CHUNKS - 1, True)
        make_mix(near, 0)

        def one(c, carry):
            send_part(near, 0, c, True)
            return carry

        lax.fori_loop(0, CHUNKS, one, 0)

    def fin_copy(c):
        return pltpu.make_async_copy(fin.at[c % 2], out_hbm.at[:, pl.ds(c * width, width)], fin_sem.at[c % 2])

    make_mix(p, 0)
    for c in range(CHUNKS):
        hid_copy = pltpu.make_async_copy(hidden_hbm.at[:, pl.ds(c * width, width)], hid, hid_sem)
        hid_copy.start()
        returned(p, c)
        hid_copy.wait()

        def own(here):
            hid[here] = hid[here] + combine(p, 0, c, here)

        by_rows(own)

        @pl.when(inner)
        def _():
            part_arrival(p, c).wait_recv()
            part_arrival(PLANES, c).wait_recv()

            def step(here):
                both = parts[p, c, here].astype(f32) + parts[PLANES, c, here].astype(f32)
                fin[c % 2, here] = (hid[here] + both).astype(bf16)

            by_rows(step)

        @pl.when(jnp.logical_not(inner))
        def _():
            index = jnp.where(first, PLANES, p)
            part_arrival(index, c).wait_recv()

            def step(here):
                fin[c % 2, here] = (hid[here] + parts[index, c, here].astype(f32)).astype(bf16)

            by_rows(step)

        fin_copy(c).start()
        if c:
            fin_copy(c - 1).wait()
    fin_copy(CHUNKS - 1).wait()

    for way in range(2):

        @pl.when(ways[way])
        def _():
            for c in range(CHUNKS + 1):
                own_copy(way, c).wait_send()

    def drain(k, carry):
        s = lookup(ORDER, p, k)
        for d in range(rest - 1):
            for c in range(CHUNKS):
                away_copy(s, d, c).wait_send()
                back_copy(s, d, c).wait_send()

        @pl.when(k > 0)
        def _():
            for c in range(CHUNKS):
                part_copy(s, c).wait_send()

        @pl.when((k > 0) & inner)
        def _():
            meta_copy(s, meta_send.at[s], below).wait_send()

        return carry

    lax.fori_loop(0, PLANES, drain, 0)


def experts_and_back(normed, meta, hidden, w_gate, w_up, w_down):
    rest = lax.axis_size("sp") // PLANES
    experts, model, ffe = w_gate.shape
    tokens = normed.shape[0]
    width = model // CHUNKS
    dma = pltpu.SemaphoreType.DMA
    anywhere = pl.BlockSpec(memory_space=pl.ANY)
    return pl.pallas_call(
        functools.partial(moe_kernel, rest),
        in_specs=[anywhere] * 6,
        out_specs=anywhere,
        out_shape=jax.ShapeDtypeStruct((tokens, model), bf16),
        scratch_shapes=[
            pltpu.VMEM((PLANES, CHUNKS, tokens, width), bf16),
            pltpu.VMEM((PLANES,) + meta.shape, f32),
            pltpu.VMEM((PLANES, rest, CHUNKS, experts, CAP, width), bf16),
            pltpu.VMEM((PLANES, rest - 1, CHUNKS, experts, CAP, width), bf16),
            pltpu.VMEM((PLANES, rest - 1, CHUNKS, experts, CAP, width), bf16),
            pltpu.VMEM((PLANES + 1, CHUNKS, tokens, width), bf16),
            pltpu.VMEM(w_gate.shape, bf16),
            pltpu.VMEM(w_up.shape, bf16),
            pltpu.VMEM(w_down.shape, bf16),
            pltpu.VMEM((rest * experts * CAP, tokens), bf16),
            pltpu.VMEM((2, rest, tokens, experts * CAP), bf16),
            pltpu.VMEM((experts, rest * CAP, ffe), bf16),
            pltpu.VMEM((tokens, width), f32),
            pltpu.VMEM((2, tokens, width), bf16),
            dma((CHUNKS,)),
            dma,
            dma((3, experts)),
            dma((2, CHUNKS)),
            dma((2,)),
            dma((PLANES, CHUNKS)),
            dma((PLANES, CHUNKS)),
            dma((PLANES,)),
            dma((PLANES,)),
            dma((PLANES, rest - 1, CHUNKS)),
            dma((PLANES, rest - 1, CHUNKS)),
            dma((PLANES, rest - 1, CHUNKS)),
            dma((PLANES, rest - 1, CHUNKS)),
            dma((PLANES, CHUNKS)),
            dma((PLANES + 1, CHUNKS)),
            dma,
            dma((2,)),
        ],
        compiler_params=pltpu.CompilerParams(collective_id=0, has_side_effects=True, vmem_limit_bytes=67043328),
        cost_estimate=pl.CostEstimate(
            flops=6 * PLANES * rest * experts * CAP * model * ffe,
            bytes_accessed=2 * (w_gate.size * 3 + 4 * normed.size),
            transcendentals=PLANES * rest * experts * CAP * ffe,
        ),
    )(normed, meta, hidden, w_gate, w_up, w_down)


def from_behind(x, axis, by):
    devices = lax.axis_size(axis)
    pairs = [(i, i + by) for i in range(devices) if 0 <= i + by < devices]
    return lax.ppermute(x, axis, pairs)


def slot_table(ids, weights, experts):
    tokens = ids.shape[1]
    names = jnp.arange(experts, dtype=jnp.int32)[:, None]
    hits = [ids[j][None, :] == names for j in range(2)]
    named = (hits[0] | hits[1]).astype(bf16)
    at = jnp.arange(tokens, dtype=jnp.int32)
    earlier = (at[:, None] < at[None, :]).astype(bf16)
    before = jnp.dot(named, earlier, preferred_element_type=f32)
    rank = [jnp.sum(jnp.where(hits[j], before, 0.0), axis=0) for j in range(2)]
    slot = [ids[j].astype(f32) * CAP + rank[j] for j in range(2)]
    return jnp.concatenate([jnp.stack(slot), weights, jnp.zeros((4, tokens), f32)], axis=0)


def per_device(
    residual_in,
    conv_input,
    input_gate,
    output_gate,
    conv_taps,
    doc_ids,
    proj_weight,
    norm_gain,
    expert_ids,
    expert_weight,
    w_gate,
    w_up,
    w_down,
):
    kernel_width = conv_taps.shape[0]
    rim_rows = kernel_width - 1
    meta = slot_table(expert_ids.T, expert_weight.T, w_gate.shape[0] * lax.axis_size("sp"))

    product = input_gate.astype(f32) * conv_input.astype(f32)
    doc_float = doc_ids.astype(f32)
    doc_rim = jnp.broadcast_to(doc_float[-rim_rows:, None], (rim_rows, 128))
    rim = from_behind(jnp.concatenate([product[-rim_rows:], doc_rim], axis=1), "sp", 1)
    channels = product.shape[1]
    prev_in, prev_ids = rim[:, :channels], rim[:, channels]
    prev_ids = jnp.where(lax.axis_index("sp") == 0, -1.0, prev_ids)
    padded_in = jnp.concatenate([prev_in, product], axis=0)
    padded_ids = jnp.concatenate([prev_ids, doc_float], axis=0)
    length = product.shape[0]
    conv_sum = jnp.zeros(product.shape, f32)
    for offset in range(kernel_width):
        same_doc = padded_ids[offset : offset + length] == doc_float
        term = conv_taps[offset].astype(f32)[None, :] * padded_in[offset : offset + length]
        conv_sum = conv_sum + jnp.where(same_doc[:, None], term, 0.0)
    gated = (output_gate.astype(f32) * conv_sum).astype(bf16)
    regrouped = lax.all_to_all(gated, "tp", split_axis=0, concat_axis=1, tiled=True)

    mixed = jnp.dot(regrouped, proj_weight, preferred_element_type=f32)
    hidden = residual_in.astype(f32) + mixed
    scale_rows = lax.rsqrt(jnp.mean(hidden * hidden, axis=-1, keepdims=True) + epsilon)
    normed = (hidden * scale_rows * norm_gain[None, :]).astype(bf16)
    return experts_and_back(normed, meta, hidden, w_gate, w_up, w_down)


def solution(mesh):
    return jax.shard_map(
        per_device,
        mesh=mesh,
        in_specs=(
            P(("sp", "tp"), None),
            P("sp", "tp"),
            P("sp", "tp"),
            P("sp", "tp"),
            P(None, "tp"),
            P("sp"),
            P(),
            P(),
            P(("sp", "tp"), None),
            P(("sp", "tp"), None),
            P("sp", None, None),
            P("sp", None, None),
            P("sp", None, None),
        ),
        out_specs=P(("sp", "tp"), None),
        check_vma=False,
    )
```

```python
import functools

import jax
import jax.numpy as jnp
from jax import lax
from jax.experimental import pallas as pl
from jax.experimental.pallas import tpu as pltpu
from jax.sharding import PartitionSpec as P

CAP = 64
PLANES = 4
CHUNKS = 4
BLOCK = 128
HALF = 256
epsilon = 1e-06
MESH = pl.DeviceIdType.MESH
bf16, f32 = jnp.bfloat16, jnp.float32


def lookup(table, p, k):
    out = 0
    for i, row in enumerate(table):
        for j, v in enumerate(row):
            out = out + jnp.where((p == i) & (k == j), v, 0)
    return out


ORDER = ((0, 1, 3, 2), (1, 0, 3, 2), (2, 3, 0, 1), (3, 2, 0, 1))
LOW = ((0, 1, 2, 3), (0, 1, 3, 3), (0, 1, 3, 3), (0, 1, 2, 3))
HIGH = ((1, 2, 2, 3), (1, 3, 3, 4), (1, 3, 3, 4), (1, 2, 2, 3))


def moe_kernel(
    rest,
    share_weights,
    share_mix,
    conv_hbm,
    entry_hbm,
    exit_hbm,
    docs_hbm,
    taps_hbm,
    routes_hbm,
    proj_hbm,
    residual_hbm,
    gain_hbm,
    gate_hbm,
    up_hbm,
    down_hbm,
    out_hbm,
    hidden_hbm,
    tok,
    meta,
    slots,
    away,
    back,
    parts,
    gate,
    up,
    down,
    pick,
    mix,
    act,
    hid,
    fin,
    taps,
    routes,
    gain,
    rim_out,
    rim_in,
    edge,
    load_sem,
    proj_sem,
    residual_sem,
    small_sem,
    rim_send,
    rim_recv,
    deal_send,
    deal_recv,
    weight_sem,
    own_sem,
    own_meta_sem,
    tok_send,
    tok_recv,
    meta_send,
    meta_recv,
    away_send,
    away_recv,
    back_send,
    back_recv,
    part_send,
    part_recv,
    hid_sem,
    fin_sem,
    *extra,
):
    me = lax.axis_index("sp")
    p, r = me // rest, lax.rem(me, rest)
    first, last = p == 0, p == PLANES - 1
    inner = jnp.logical_not(first | last)
    below = lax.max(me - rest, 0)
    above = lax.min(me + rest, PLANES * rest - 1)
    experts, _, hidden_width = gate.shape
    tokens, width = tok.shape[2], tok.shape[3]
    local = experts * CAP
    peers = [p * rest + lax.rem(r + d, rest) for d in range(1, rest)]
    origins = [p * rest + lax.rem(r + rest - d, rest) for d in range(1, rest)]

    def remote(src, dst, send, recv, device):
        return pltpu.make_async_remote_copy(
            src_ref=src, dst_ref=dst, send_sem=send, recv_sem=recv, device_id={"sp": device}, device_id_type=MESH
        )

    def token_copy(s, c, send, device):
        return remote(tok.at[s, c], tok.at[s, c], send, tok_recv.at[s, c], device)

    def meta_copy(s, send, device):
        return remote(meta.at[s], meta.at[s], send, meta_recv.at[s], device)

    def away_copy(s, d, c):
        peer = peers[d]
        return remote(slots.at[s, lax.rem(r + d + 1, rest), c], away.at[s, d, c], away_send.at[s, d, c], away_recv.at[s, d, c], peer)

    def back_copy(s, d, c):
        return remote(away.at[s, d, c], back.at[s, d, c], back_send.at[s, d, c], back_recv.at[s, d, c], origins[d])

    def part_copy(s, c):
        down_way = p > s
        target = jnp.where(down_way, below, above)
        index = jnp.where(down_way & (p - 1 == s), PLANES, s)
        return remote(tok.at[s, c], parts.at[index, c], part_send.at[s, c], part_recv.at[index, c], target)

    def part_arrival(index, c):
        return remote(tok.at[0, c], parts.at[index, c], part_send.at[0, c], part_recv.at[index, c], below)

    def weight_copies(e):
        pairs = ((gate_hbm, gate), (up_hbm, up), (down_hbm, down))
        return [pltpu.make_async_copy(a.at[e], b.at[e], weight_sem.at[i, e]) for i, (a, b) in enumerate(pairs)]

    tp_size = lax.axis_size("tp")
    t = lax.axis_index("tp")
    positions, channels = conv_hbm.shape
    depth = proj_hbm.shape[0]
    if share_weights:
        conv_in, entry = up.at[0, :, 0:channels], up.at[0, :, channels : 2 * channels]
        exit_gate, docs = up.at[1, :, 0:channels], up.at[1, :, channels : channels + 128]
        proj = [gate.at[c // 2, pl.ds((c % 2) * depth, depth), :] for c in range(CHUNKS)]

        def gated(j):
            return down.at[j, :, width : width + channels]

    else:
        conv_s, docs_s, proj_s, gated_s = extra[:4]
        conv_in, entry, exit_gate, docs = conv_s.at[0], conv_s.at[1], conv_s.at[2], docs_s
        proj = [proj_s.at[c] for c in range(CHUNKS)]

        def gated(j):
            return gated_s.at[j]

    def dealt(j):
        return mix.at[j // rest, lax.rem(j, rest)] if share_mix else extra[-1].at[j]

    def deal_copy(offset):
        j = lax.rem(t + offset, tp_size)
        return pltpu.make_async_remote_copy(
            src_ref=gated(j),
            dst_ref=dealt(t),
            send_sem=deal_send.at[offset],
            recv_sem=deal_recv.at[t],
            device_id={"tp": j},
            device_id_type=MESH,
        )

    def deal_arrival(offset):
        j = lax.rem(t + tp_size - offset, tp_size)
        return pltpu.make_async_remote_copy(
            src_ref=gated(j),
            dst_ref=dealt(j),
            send_sem=deal_send.at[offset],
            recv_sem=deal_recv.at[j],
            device_id={"tp": j},
            device_id_type=MESH,
        )

    sources = ((conv_hbm, conv_in), (entry_hbm, entry), (docs_hbm, docs), (exit_hbm, exit_gate))
    loads = [pltpu.make_async_copy(a, b, load_sem.at[i]) for i, (a, b) in enumerate(sources)]
    smalls = [
        pltpu.make_async_copy(a, b, small_sem.at[i])
        for i, (a, b) in enumerate(((taps_hbm, taps), (routes_hbm, routes), (gain_hbm, gain)))
    ]
    proj_loads = [
        pltpu.make_async_copy(proj_hbm.at[:, pl.ds(c * width, width)], proj[c], proj_sem.at[c]) for c in range(CHUNKS)
    ]
    residual_loads = [
        pltpu.make_async_copy(residual_hbm.at[:, pl.ds(c * width, width)], tok.at[p, c], residual_sem.at[c])
        for c in range(CHUNKS)
    ]
    for load in loads + smalls + proj_loads + residual_loads:
        load.start()

    devices = PLANES * rest
    final_device = me == devices - 1
    behind, ahead = lax.max(me - 1, 0), lax.min(me + 1, devices - 1)
    barrier = pltpu.get_barrier_semaphore()
    greetings = ((jnp.logical_not(first), below), (jnp.logical_not(last), above), (me > 0, behind), (me < devices - 1, ahead))
    for there, device in greetings:

        @pl.when(there)
        def _():
            pl.semaphore_signal(barrier, inc=1, device_id={"sp": device}, device_id_type=MESH)

    for peer in peers:
        pl.semaphore_signal(barrier, inc=1, device_id={"sp": peer}, device_id_type=MESH)
    for offset in range(1, tp_size):
        pl.semaphore_signal(barrier, inc=1, device_id={"tp": lax.rem(t + offset, tp_size)}, device_id_type=MESH)
    line = jnp.where(inner, 2, 1) + jnp.where((me == 0) | final_device, 1, 2)
    pl.semaphore_wait(barrier, rest - 1 + tp_size - 1 + line)

    for load in loads[:3]:
        load.wait()
    smalls[0].wait()
    rim = remote(rim_out, rim_in, rim_send, rim_recv, ahead)

    def tail(base):
        rows = pl.ds(pl.multiple_of(base - 16, 16), 16)
        return (conv_in[rows, :].astype(f32) * entry[rows, :].astype(f32))[8:], docs[rows, :].astype(f32)[8:]

    rim_values, rim_docs = tail(positions)
    rim_out[:, :channels] = rim_values
    rim_out[:, channels:] = rim_docs

    @pl.when(me < devices - 1)
    def _():
        rim.start()

    @pl.when(me == 0)
    def _():
        rim_in[:, :channels] = jnp.zeros((8, channels), f32)
        rim_in[:, channels:] = jnp.full((8, 128), -1.0, f32)

    loads[3].wait()

    def conv_block(j, target):
        @pl.when((j == 0) & (me > 0))
        def _():
            rim.wait_recv()

        def piece(b, carry):
            base = j * tokens + b * BLOCK
            rows = pl.ds(pl.multiple_of(base, BLOCK), BLOCK)
            value = conv_in[rows, :].astype(f32) * entry[rows, :].astype(f32)
            doc = docs[rows, :].astype(f32)

            @pl.when(base == 0)
            def _():
                edge[...] = rim_in[...]

            @pl.when(base > 0)
            def _():
                edge[:, :channels], edge[:, channels:] = tail(base)

            long = jnp.concatenate([edge[:, :channels], value], axis=0)
            long_docs = jnp.concatenate([edge[:, channels:], doc], axis=0)
            total = jnp.zeros((BLOCK, channels), f32)
            reach = taps.shape[0] - 1
            for k in range(reach + 1):
                term = taps[k : k + 1, :].astype(f32) * long[8 - reach + k : 8 - reach + k + BLOCK]
                if k < reach:
                    same = jnp.where(long_docs[8 - reach + k : 8 - reach + k + BLOCK] == doc, 1.0, 0.0)
                    term = term * jnp.concatenate([same] * (channels // 128), axis=1)
                total = total + term
            target[pl.ds(pl.multiple_of(b * BLOCK, BLOCK), BLOCK), :] = (
                exit_gate[rows, :].astype(f32) * total
            ).astype(bf16)
            return carry

        lax.fori_loop(0, tokens // BLOCK, piece, 0)

    for offset in sorted(range(1, tp_size), key=lambda o: abs(2 * o - tp_size)):
        j = lax.rem(t + offset, tp_size)
        conv_block(j, gated(j))
        deal_copy(offset).start()
    conv_block(t, dealt(t))

    smalls[1].wait()
    names = lax.broadcasted_iota(jnp.int32, (devices * experts, tokens), 0).astype(f32)
    hits = [jnp.where(names == routes[i : i + 1, :], 1.0, 0.0) for i in range(2)]

    def earlier(q, carry):
        row = lax.broadcasted_iota(jnp.int32, (BLOCK, tokens), 0) + q * BLOCK
        column = lax.broadcasted_iota(jnp.int32, (BLOCK, tokens), 1)
        pick[pl.ds(pl.multiple_of(q * BLOCK, BLOCK), BLOCK), :] = jnp.where(row < column, 1.0, 0.0).astype(bf16)
        return carry

    lax.fori_loop(0, tokens // BLOCK, earlier, 0)
    before = jnp.dot((hits[0] + hits[1]).astype(bf16), pick[0:tokens, :], preferred_element_type=f32)
    for i in range(2):
        rank = jnp.sum(hits[i] * before, axis=0, keepdims=True)
        meta[p, i : i + 1, :] = routes[i : i + 1, :] * CAP + rank
    meta[p, 2:8, :] = routes[2:8, :]

    def own_copy(way, c):
        device = (above, below)[way]
        if c == 0:
            return meta_copy(p, own_meta_sem.at[way], device)
        return token_copy(p, c - 1, own_sem.at[way, c - 1], device)

    ways = (jnp.logical_not(last), jnp.logical_not(first))
    middle = (p == 1, p == PLANES - 2)

    def start_own(c):
        for way in range(2):

            @pl.when(ways[way] if c < 2 else ways[way] & jnp.logical_not(middle[way]))
            def _():
                own_copy(way, c).start()

    start_own(0)
    smalls[2].wait()
    for load in proj_loads + residual_loads:
        load.wait()
    for offset in range(1, tp_size):
        deal_arrival(offset).wait_recv()
    blocks = tokens // BLOCK

    def hidden_copy(q):
        return pltpu.make_async_copy(hid.at[lax.rem(q, 2), 0:CHUNKS], hidden_hbm.at[:, q], hid_sem.at[lax.rem(q, 2)])

    def project(q, carry):
        rows = pl.ds(pl.multiple_of(q * BLOCK, BLOCK), BLOCK)
        slot = lax.rem(q, 2)

        @pl.when(q > 1)
        def _():
            hidden_copy(q - 2).wait()

        squares = jnp.zeros((BLOCK, 1), f32)
        for c in range(CHUNKS):
            acc = tok[p, c, rows].astype(f32)
            for j in range(tp_size):
                weights = proj[c][pl.ds(j * channels, channels), :]
                acc = acc + jnp.dot(dealt(j)[rows, :], weights, preferred_element_type=f32)
            hid[slot, c] = acc
            squares = squares + jnp.sum(acc * acc, axis=1, keepdims=True)
        scale = lax.rsqrt(squares * (1.0 / (CHUNKS * width)) + epsilon)
        for c in range(CHUNKS):
            normed = hid[slot, c] * scale * gain[:, c * width : (c + 1) * width]
            tok[p, c, rows] = normed.astype(bf16)
        hidden_copy(q).start()
        return carry

    lax.fori_loop(0, blocks, project, 0)
    for c in range(1, CHUNKS + 1):
        start_own(c)
    for offset in range(1, tp_size):
        deal_copy(offset).wait_send()
    for q in range(max(blocks - 2, 0), blocks):
        hidden_copy(q).wait()

    @pl.when(me < devices - 1)
    def _():
        rim.wait_send()

    for e in range(experts):
        for copy in weight_copies(e):
            copy.start()

    def unpack_start(k):
        s = lookup(ORDER, p, k)
        onward = jnp.where(s < p, above, below)
        fresh = k > 0

        @pl.when(fresh)
        def _():
            meta_copy(s, meta_send.at[s], onward).wait_recv()

        @pl.when(fresh & inner)
        def _():
            meta_copy(s, meta_send.at[s], onward).start()

        def pick_rows(q, carry):
            base = (p * rest * local + q * BLOCK).astype(f32)
            names = lax.broadcasted_iota(jnp.int32, (BLOCK, tokens), 0).astype(f32)
            hit = (names == meta[s, 0:1] - base) | (names == meta[s, 1:2] - base)
            pick[pl.ds(pl.multiple_of(q * BLOCK, BLOCK), BLOCK), :] = jnp.where(hit, 1.0, 0.0).astype(bf16)
            return carry

        lax.fori_loop(0, rest * local // BLOCK, pick_rows, 0)

    def unpack_chunk(k, c):
        s = lookup(ORDER, p, k)
        onward = jnp.where(s < p, above, below)
        fresh = k > 0

        @pl.when(fresh)
        def _():
            token_copy(s, c, tok_send.at[s, c], onward).wait_recv()

        @pl.when(fresh & inner)
        def _():
            token_copy(s, c, tok_send.at[s, c], onward).start()

        def pack(q, carry):
            chosen = pick[pl.ds(pl.multiple_of(q * local, local), local), :]
            rows = jnp.dot(chosen, tok[s, c], preferred_element_type=f32).astype(bf16)
            slots[s, q, c] = rows.reshape(experts, CAP, width)
            return carry

        lax.fori_loop(0, rest, pack, 0)
        for d in range(rest - 1):
            away_copy(s, d, c).start()

    def unpack_step(k, carry):
        unpack_start(k)

        def chunk(c, carry):
            unpack_chunk(k, c)
            return carry

        lax.fori_loop(0, CHUNKS, chunk, 0)
        for way in range(2):

            @pl.when(middle[way] & (k == 1))
            def _():
                for c in range(2, CHUNKS + 1):
                    own_copy(way, c).start()

        return carry

    def expert_step(k):
        s = lookup(ORDER, p, k)
        for d in range(rest - 1):
            for c in range(CHUNKS):
                away_copy(s, d, c).wait_recv()

        def one(e, carry):
            @pl.when(k == 1)
            def _():
                for copy in weight_copies(e):
                    copy.wait()

            gate_val = jnp.zeros((rest * CAP, hidden_width), f32)
            up_val = jnp.zeros((rest * CAP, hidden_width), f32)
            for c in range(CHUNKS):
                x = jnp.concatenate([slots[s, r, c, e]] + [away[s, d, c, e] for d in range(rest - 1)], axis=0)
                rows = pl.ds(c * width, width)
                gate_val = gate_val + jnp.dot(x, gate[e, rows, :], preferred_element_type=f32)
                up_val = up_val + jnp.dot(x, up[e, rows, :], preferred_element_type=f32)
            act[e] = (gate_val * jax.nn.sigmoid(gate_val) * up_val).astype(bf16)
            return carry

        lax.fori_loop(0, experts, one, 0)

        def two(c, carry):
            for e in range(experts):
                columns = pl.ds(pl.multiple_of(c * width, width), width)
                out = jnp.dot(act[e], down[e, :, columns], preferred_element_type=f32).astype(bf16)
                slots[s, r, c, e] = out[:CAP]
                for d in range(rest - 1):
                    away[s, d, c, e] = out[(d + 1) * CAP : (d + 2) * CAP]

            @pl.when(k > 0)
            def _():
                for d in range(rest - 1):
                    back_copy(s, d, c).start()

            return carry

        lax.fori_loop(0, CHUNKS, two, 0)

    def make_mix(s, i):
        def rows(q, carry):
            here = pl.ds(pl.multiple_of(q * BLOCK, BLOCK), BLOCK)
            info = meta[s, :, here].T
            names = lax.broadcasted_iota(jnp.int32, (BLOCK, local), 1).astype(f32)
            for d in range(rest):
                base = (p * rest * local + lax.rem(r + d, rest) * local).astype(f32)
                mix[i, d, here] = (
                    jnp.where(names == info[:, 0:1] - base, info[:, 2:3], 0.0)
                    + jnp.where(names == info[:, 1:2] - base, info[:, 3:4], 0.0)
                ).astype(bf16)
            return carry

        lax.fori_loop(0, tokens // BLOCK, rows, 0)

    def returned(s, c):
        for d in range(rest - 1):
            back_copy(s, d, c).wait_recv()

    def combine(s, i, c, here):
        acc = jnp.dot(mix[i, 0, here], slots[s, r, c].reshape(local, width), preferred_element_type=f32)
        for d in range(rest - 1):
            acc = acc + jnp.dot(mix[i, d + 1, here], back[s, d, c].reshape(local, width), preferred_element_type=f32)
        return acc

    def by_rows(step):
        def body(q, carry):
            step(pl.ds(pl.multiple_of(q * HALF, HALF), HALF))
            return carry

        lax.fori_loop(0, tokens // HALF, body, 0)

    def send_part(s, i, c, passed):
        returned(s, c)
        if passed:
            part_arrival(s, c).wait_recv()
            token_copy(s, c, tok_send.at[s, c], below).wait_send()

        def step(here):
            acc = combine(s, i, c, here)
            if passed:
                acc = acc + parts[s, c, here].astype(f32)
            tok[s, c, here] = acc.astype(bf16)

        by_rows(step)
        part_copy(s, c).start()

    near = jnp.clip(PLANES - 1 - p, 0, PLANES - 1)
    end = jnp.where(p == 1, PLANES - 1, 0)
    far = PLANES - 1 - end

    def main_step(k, carry):
        lax.fori_loop(lookup(LOW, p, k), lookup(HIGH, p, k), unpack_step, 0)

        @pl.when(inner & (k == PLANES - 1))
        def _():
            make_mix(end, 0)
            make_mix(far, 1)
            send_part(end, 0, 0, True)
            send_part(end, 0, 1, True)
            send_part(far, 1, 0, True)

        def expert_turn(i, carry):
            expert_step(jnp.where(i == 0, k, 0))
            return carry

        own_turn = jnp.where(inner, PLANES - 1, 1)
        lax.fori_loop(0, jnp.where(k == own_turn, 2, 1), expert_turn, 0)

        @pl.when(k == PLANES - 1)
        def _():
            for c in range(CHUNKS):
                for d in range(rest - 1):
                    back_copy(p, d, c).start()

        @pl.when(jnp.logical_not(inner))
        def _():
            s = lookup(ORDER, p, k)
            make_mix(s, 0)

            @pl.when(k < PLANES - 1)
            def _():
                unpack_start(k + 1)

            def chunk(c, carry):
                @pl.when(k < PLANES - 1)
                def _():
                    unpack_chunk(k + 1, c)

                send_part(s, 0, c, False)
                return carry

            lax.fori_loop(0, CHUNKS, chunk, 0)

        return carry

    unpack_step(0, 0)
    lax.fori_loop(1, PLANES, main_step, 0)

    @pl.when(inner)
    def _():
        def two(c, carry):
            send_part(end, 0, c, True)
            send_part(far, 1, c - 1, True)
            return carry

        lax.fori_loop(2, CHUNKS, two, 0)
        send_part(far, 1, CHUNKS - 1, True)
        make_mix(near, 0)

        def one(c, carry):
            send_part(near, 0, c, True)
            return carry

        lax.fori_loop(0, CHUNKS, one, 0)

    def fin_copy(c):
        return pltpu.make_async_copy(fin, out_hbm.at[:, pl.ds(c * width, width)], fin_sem)

    def hid_load(c):
        return pltpu.make_async_copy(hidden_hbm.at[c], hid.at[c % 2, 0:blocks], hid_sem.at[c % 2])

    def piece(c, here):
        return hid[c % 2, pl.ds(here.start // BLOCK, HALF // BLOCK)].reshape(HALF, width)

    make_mix(p, 0)
    hid_load(0).start()
    for c in range(CHUNKS):
        hid_load(c).wait()
        if c + 1 < CHUNKS:
            hid_load(c + 1).start()
        returned(p, c)

        def own(here):
            total = piece(c, here) + combine(p, 0, c, here)
            hid[c % 2, pl.ds(here.start // BLOCK, HALF // BLOCK)] = total.reshape(HALF // BLOCK, BLOCK, width)

        by_rows(own)
        if c:
            fin_copy(c - 1).wait()

        @pl.when(inner)
        def _():
            part_arrival(p, c).wait_recv()
            part_arrival(PLANES, c).wait_recv()

            def step(here):
                both = parts[p, c, here].astype(f32) + parts[PLANES, c, here].astype(f32)
                fin[here] = (piece(c, here) + both).astype(bf16)

            by_rows(step)

        @pl.when(jnp.logical_not(inner))
        def _():
            index = jnp.where(first, PLANES, p)
            part_arrival(index, c).wait_recv()

            def step(here):
                fin[here] = (piece(c, here) + parts[index, c, here].astype(f32)).astype(bf16)

            by_rows(step)

        fin_copy(c).start()
    fin_copy(CHUNKS - 1).wait()

    for way in range(2):

        @pl.when(ways[way])
        def _():
            for c in range(CHUNKS + 1):
                own_copy(way, c).wait_send()

    def drain(k, carry):
        s = lookup(ORDER, p, k)
        for d in range(rest - 1):
            for c in range(CHUNKS):
                away_copy(s, d, c).wait_send()
                back_copy(s, d, c).wait_send()

        @pl.when(k > 0)
        def _():
            for c in range(CHUNKS):
                part_copy(s, c).wait_send()

        @pl.when((k > 0) & inner)
        def _():
            meta_copy(s, meta_send.at[s], below).wait_send()

        return carry

    lax.fori_loop(0, PLANES, drain, 0)


def layer(conv_input, input_gate, output_gate, docs, taps, routes, proj, residual, gain, w_gate, w_up, w_down):
    rest = lax.axis_size("sp") // PLANES
    tp_size = lax.axis_size("tp")
    experts, model, ffe = w_gate.shape
    tokens = residual.shape[0]
    positions, channels = conv_input.shape
    depth = proj.shape[0]
    width = model // CHUNKS
    pieces = max(CHUNKS, tokens // BLOCK)
    dma = pltpu.SemaphoreType.DMA
    anywhere = pl.BlockSpec(memory_space=pl.ANY)
    share_weights = (
        experts >= max(CHUNKS, tp_size)
        and (model, ffe, ffe) == (positions, width, tokens)
        and 2 * depth <= model
        and 2 * channels <= ffe
        and channels >= 128
        and width + channels <= model
    )
    share_mix = tp_size == 2 * rest and channels == experts * CAP
    extra = []
    if not share_weights:
        extra += [
            pltpu.VMEM((3, positions, channels), bf16),
            pltpu.VMEM(docs.shape, bf16),
            pltpu.VMEM((CHUNKS, depth, width), bf16),
            pltpu.VMEM((tp_size, tokens, channels), bf16),
        ]
    if not share_mix:
        extra += [pltpu.VMEM((tp_size, tokens, channels), bf16)]
    return pl.pallas_call(
        functools.partial(moe_kernel, rest, share_weights, share_mix),
        in_specs=[anywhere] * 12,
        out_specs=[anywhere] * 2,
        out_shape=[
            jax.ShapeDtypeStruct((tokens, model), bf16),
            jax.ShapeDtypeStruct((CHUNKS, tokens // BLOCK, BLOCK, width), f32),
        ],
        scratch_shapes=[
            pltpu.VMEM((PLANES, CHUNKS, tokens, width), bf16),
            pltpu.VMEM((PLANES,) + routes.shape, f32),
            pltpu.VMEM((PLANES, rest, CHUNKS, experts, CAP, width), bf16),
            pltpu.VMEM((PLANES, rest - 1, CHUNKS, experts, CAP, width), bf16),
            pltpu.VMEM((PLANES, rest - 1, CHUNKS, experts, CAP, width), bf16),
            pltpu.VMEM((PLANES + 1, CHUNKS, tokens, width), bf16),
            pltpu.VMEM(w_gate.shape, bf16),
            pltpu.VMEM(w_up.shape, bf16),
            pltpu.VMEM(w_down.shape, bf16),
            pltpu.VMEM((rest * experts * CAP, tokens), bf16),
            pltpu.VMEM((2, rest, tokens, experts * CAP), bf16),
            pltpu.VMEM((experts, rest * CAP, ffe), bf16),
            pltpu.VMEM((2, pieces, BLOCK, width), f32),
            pltpu.VMEM((tokens, width), bf16),
            pltpu.VMEM(taps.shape, bf16),
            pltpu.VMEM(routes.shape, f32),
            pltpu.VMEM(gain.shape, f32),
            pltpu.VMEM((8, channels + 128), f32),
            pltpu.VMEM((8, channels + 128), f32),
            pltpu.VMEM((8, channels + 128), f32),
            dma((4,)),
            dma((CHUNKS,)),
            dma((CHUNKS,)),
            dma((3,)),
            dma,
            dma,
            dma((tp_size,)),
            dma((tp_size,)),
            dma((3, experts)),
            dma((2, CHUNKS)),
            dma((2,)),
            dma((PLANES, CHUNKS)),
            dma((PLANES, CHUNKS)),
            dma((PLANES,)),
            dma((PLANES,)),
            dma((PLANES, rest - 1, CHUNKS)),
            dma((PLANES, rest - 1, CHUNKS)),
            dma((PLANES, rest - 1, CHUNKS)),
            dma((PLANES, rest - 1, CHUNKS)),
            dma((PLANES, CHUNKS)),
            dma((PLANES + 1, CHUNKS)),
            dma((2,)),
            dma,
        ]
        + extra,
        compiler_params=pltpu.CompilerParams(collective_id=0, has_side_effects=True, vmem_limit_bytes=67043328),
        cost_estimate=pl.CostEstimate(
            flops=6 * PLANES * rest * experts * CAP * model * ffe,
            bytes_accessed=2 * (w_gate.size * 3 + 4 * residual.size),
            transcendentals=PLANES * rest * experts * CAP * ffe,
        ),
    )(conv_input, input_gate, output_gate, docs, taps, routes, proj, residual, gain, w_gate, w_up, w_down)[0]


def per_device(
    residual_in,
    conv_input,
    input_gate,
    output_gate,
    conv_taps,
    doc_ids,
    proj_weight,
    norm_gain,
    expert_ids,
    expert_weight,
    w_gate,
    w_up,
    w_down,
):
    tokens = expert_ids.shape[0]
    routes = jnp.concatenate([expert_ids.T.astype(f32), expert_weight.T, jnp.zeros((4, tokens), f32)], axis=0)
    docs = jnp.broadcast_to(doc_ids.astype(bf16)[:, None], (doc_ids.shape[0], 128))
    gain = norm_gain[None, :]
    return layer(
        conv_input, input_gate, output_gate, docs, conv_taps, routes, proj_weight, residual_in, gain, w_gate, w_up, w_down
    )


def solution(mesh):
    return jax.shard_map(
        per_device,
        mesh=mesh,
        in_specs=(
            P(("sp", "tp"), None),
            P("sp", "tp"),
            P("sp", "tp"),
            P("sp", "tp"),
            P(None, "tp"),
            P("sp"),
            P(),
            P(),
            P(("sp", "tp"), None),
            P(("sp", "tp"), None),
            P("sp", None, None),
            P("sp", None, None),
            P("sp", None, None),
        ),
        out_specs=P(("sp", "tp"), None),
        check_vma=False,
    )
```
